32 devices in a mesh: sp: 8 (over z, y), tp: 4 (over x, core).
Axes of the slice: x: 2, y: 2, z: 4, core: 2. Of those that a mesh axis runs over, the one named last changes fastest.
Arguments:
- resid: bfloat16 [6144, 4096], P(('sp', 'tp')), may hold values from -80 to 80
- pool_in: bfloat16 [6144, 1024], P('sp', 'tp'), may hold values from -6 to 6
- pool_weight: bfloat16 [4, 256, 256], P('tp'), may hold values from -0.375 to 0.375
- pool_scale: float32 [1024], P('tp'), may hold values from 0.1 to 1.9
- out_weight: bfloat16 [1024, 4096], P('tp'), may hold values from -0.1875 to 0.1875
- norm_gain: float32 [4096], replicated, may hold values from 0.1 to 1.9
- route_ids: int32 [6144, 4], P(('sp', 'tp')), may hold values from 0 to 31, all different within a row; in each aligned block of 192 rows (0 to 191, 192 to 383, ...) at most 36 rows name the same one
- route_weight: float32 [6144, 4], P(('sp', 'tp')), may hold values from 0.1 to 1
- expert_gate: bfloat16 [32, 4096, 384], P('sp'), may hold values from -0.09375 to 0.09375
- expert_up: bfloat16 [32, 4096, 384], P('sp'), may hold values from -0.09375 to 0.09375
- expert_down: bfloat16 [32, 384, 4096], P('sp'), may hold values from -0.3125 to 0.3125
- shared_gate: bfloat16 [4096, 384], replicated, may hold values from -0.09375 to 0.09375
- shared_up: bfloat16 [4096, 384], replicated, may hold values from -0.09375 to 0.09375
- shared_down: bfloat16 [384, 4096], replicated, may hold values from -0.3125 to 0.3125
Outputs:
- layer_out: bfloat16 [6144, 4096], P(('sp', 'tp'))
The draws below stay inside these ranges and needn't reach their ends.
Inputs may be any that keep to these rules, and one draw needn't show every extreme that they name: `route_ids`: each row names 4 different experts. Among the rows of one device no expert is named more than 36 times, and that count is reached.
All inputs are finite; a program needn't handle non-finite values.
Results may differ from the reference program's by a relative error of at most 0.012.
Values may be sent and summed in bfloat16 or wider, within the bound.
A program may use at most 192 MiB of HBM per device.

```python
import math
import jax
import jax.numpy as jnp
import numpy as np
from jax import lax

D = 4096
POOL_WIDTH = 1024
POOL_GROUP = 256
FE = 384
FS = 384
EXPERTS = 32
TOP_K = 4
TOK_DEV = 768
TOKENS = 6144
CAP = 36
N_SP = 8
N_TP = 4


def draw_resid(key, part):
    base = jnp.clip(jax.random.normal(jax.random.fold_in(key, 11), (TOKENS, D), jnp.float32), -6.0, 6.0)
    column_scale = 0.3 * 10.0 ** jax.random.uniform(jax.random.fold_in(key, 12), (D,), jnp.float32)
    return (base * column_scale[None, :]).astype(jnp.bfloat16)


def steps_of(stream_key, shape, cuts, least, high):
    gain, own = 1.0, jax.random.fold_in(stream_key, 6)
    for position, blocks in cuts:
        steps = jnp.exp(jax.random.uniform(jax.random.fold_in(own, position), (blocks,), jnp.float32, least / len(cuts), high / len(cuts)))
        gain = gain * jnp.repeat(steps, shape[position] // blocks).reshape([-1 if axis == position else 1 for axis in range(len(shape))])
    return gain


def assign_block(key, own, number, rows, amount, top, most, lean):
    ranking = jax.random.permutation(key, amount)
    crowded, ordinary = portions_of(amount, rows * top, most, lean, True), portions_of(amount, rows * top, most, lean, False)
    places = jnp.arange(amount)

    def named(sizes, turn):
        used = int((sizes > 0).sum())
        fixed = max(1, used // 4)
        moved = fixed + (places - fixed + turn * (used - fixed)) % max(1, amount - fixed)
        return jnp.zeros((amount,), jnp.int32).at[ranking[jnp.where(places < fixed, places, moved)]].set(jnp.asarray(sizes, jnp.int32))

    sizes = jnp.where(number % 4 == 0, named(crowded, number // 4), named(ordinary, number - number // 4 - 1))
    mixed = jax.random.permutation(jax.random.fold_in(own, 3), amount)
    source_of, receiver = mixed[0:amount // 2 * 2:2], mixed[1:amount // 2 * 2:2]
    margin = jnp.minimum(sizes[source_of] - 1, most - sizes[receiver]) // 2
    margin = jnp.where((source_of == ranking[0]) | (receiver == ranking[0]) | (sizes[receiver] == 0), 0, jnp.maximum(margin, 0))
    moved = jax.random.randint(jax.random.fold_in(own, 4), (amount // 2,), 0, 1 << 20) % (margin + 1)
    sizes = sizes.at[source_of].add(-moved).at[receiver].add(moved)
    labels = jnp.searchsorted(jnp.cumsum(sizes), jnp.arange(rows * top), side="right").astype(jnp.int32)
    grid = labels.reshape(top, rows).T
    grid = grid[jax.random.permutation(jax.random.fold_in(own, 1), rows)]
    turn = jax.random.randint(jax.random.fold_in(own, 2), (rows, 1), 0, top)
    return jnp.take_along_axis(grid, (jnp.arange(top)[None, :] + turn) % top, axis=1)


def portions_of(number_of, total, bound, lean, full):
    loads = [(1 << 20) // math.isqrt(standing ** lean) + 1 for standing in range(1, number_of + 1)]
    largest = bound if full else min(bound, max(-(-total // number_of), total * loads[0] // sum(loads)))
    least = 1 if total - largest >= number_of - 1 else 0
    given, spare = [largest] + [least] * (number_of - 1), total - largest - least * (number_of - 1)
    while spare > 0:
        candidates = [i for i in range(1, number_of) if given[i] < largest] or [i for i in range(1, number_of) if given[i] < bound]
        whole, budget = sum([loads[i] for i in candidates]), spare
        for i in candidates:
            extra = min(bound - given[i], max(1, budget * loads[i] // whole), spare)
            given[i] = given[i] + extra
            spare = spare - extra
    return np.array(given)


def noise(stream_key, shape, scale, bound, shards=(), held_as=jnp.bfloat16):
    loudness = steps_of(stream_key, shape, shards, -0.22, 0.18) if shards else 1.0
    values = jax.random.normal(stream_key, shape, jnp.float32) * scale * loudness
    return jnp.minimum(jnp.maximum(values, -bound), bound).astype(held_as)


def setup_inputs(seed: int = 0) -> dict:
    seeds = jax.random.split(jax.random.key(seed), 15)
    resid = draw_resid(jax.random.fold_in(seeds[14], 71), 0)
    pool_in = noise(seeds[1], (TOKENS, POOL_WIDTH), 1.0, 6.0, ((0, 8), (1, 4)))
    pool_weight = noise(seeds[2], (4, POOL_GROUP, POOL_GROUP), POOL_GROUP ** -0.5, 0.375, ((0, 4),))
    pool_scale = jnp.clip(1.0 + 0.18 * jax.random.normal(seeds[3], (POOL_WIDTH,), jnp.float32), 0.1, 1.9)
    out_weight = noise(seeds[4], (POOL_WIDTH, D), POOL_WIDTH ** -0.5, 0.1875, ((0, 4),))
    norm_gain = jnp.clip(1.0 + 0.18 * jax.random.normal(seeds[5], (D,), jnp.float32), 0.1, 1.9)
    route_ids_keys = jax.random.split(jax.random.fold_in(seeds[6], 1), TOKENS // (TOK_DEV // N_TP))
    route_ids_turns = jax.random.permutation(jax.random.fold_in(seeds[6], 3), TOKENS // (TOK_DEV // N_TP))
    route_ids = jax.vmap(lambda own, number: assign_block(jax.random.fold_in(seeds[6], 2), own, number, TOK_DEV // N_TP, EXPERTS, TOP_K, CAP, 1))(route_ids_keys, route_ids_turns).reshape((TOKENS, TOP_K))
    route_weight = jnp.clip(jnp.exp(math.log(1.0) - 2.3025851 * jax.random.uniform(seeds[7], (TOKENS, TOP_K), jnp.float32) ** steps_of(seeds[7], (TOKENS, TOP_K), ((0, 32),), -0.2, 0.2)), 0.1, 1.0)
    expert_gate = noise(seeds[8], (EXPERTS, D, FE), D ** -0.5, 0.09375, ((0, 8),))
    expert_up = noise(seeds[9], (EXPERTS, D, FE), D ** -0.5, 0.09375, ((0, 8),))
    expert_down = noise(seeds[10], (EXPERTS, FE, D), FE ** -0.5, 0.3125, ((0, 8),))
    shared_gate = noise(seeds[11], (D, FS), D ** -0.5, 0.09375)
    shared_up = noise(seeds[12], (D, FS), D ** -0.5, 0.09375)
    shared_down = noise(seeds[13], (FS, D), FS ** -0.5, 0.3125)
    return {"resid": resid, "pool_in": pool_in, "pool_weight": pool_weight, "pool_scale": pool_scale, "out_weight": out_weight, "norm_gain": norm_gain, "route_ids": route_ids, "route_weight": route_weight, "expert_gate": expert_gate, "expert_up": expert_up, "expert_down": expert_down, "shared_gate": shared_gate, "shared_up": shared_up, "shared_down": shared_down}


def pool_mix(pool_in, pool_weight, pool_scale):
    whole_len = pool_in.shape[0]
    group_width = pool_weight.shape[1]
    padded = jnp.pad(pool_in.astype(jnp.float32), ((8, 8), (0, 0)))
    positions = jnp.arange(whole_len, dtype=jnp.int32)
    outputs = []
    for group_num in range(4):
        half_span = 2 ** group_num
        columns = padded[:, group_num * group_width:(group_num + 1) * group_width]
        running = jnp.zeros((whole_len, group_width), jnp.float32)
        for row_shift in range(-half_span, half_span):
            running = running + columns[8 + row_shift:8 + row_shift + whole_len]
        upper_end = jnp.minimum(positions + half_span, whole_len)
        lower_end = jnp.maximum(positions - half_span, 0)
        row_count = (upper_end - lower_end).astype(jnp.float32)
        center = columns[8:8 + whole_len]
        spread = (running / row_count[:, None] - center).astype(jnp.bfloat16)
        outputs.append(jnp.dot(spread, pool_weight[group_num], preferred_element_type=jnp.float32))
    mixed_rows = jnp.concatenate(outputs, axis=1)
    return (mixed_rows * pool_scale[None, :]).astype(jnp.bfloat16)

def reference(resid, pool_in, pool_weight, pool_scale, out_weight, norm_gain, route_ids, route_weight, expert_gate, expert_up, expert_down, shared_gate, shared_up, shared_down):
    pooled = pool_mix(pool_in, pool_weight, pool_scale)
    middle = (resid.astype(jnp.float32) + jnp.dot(pooled, out_weight, preferred_element_type=jnp.float32)).astype(jnp.bfloat16)
    middle_float = middle.astype(jnp.float32)
    square_mean = lax.optimization_barrier(jnp.mean(middle_float * middle_float, axis=1, keepdims=True))
    normed = (middle_float * lax.rsqrt(square_mean + 1e-06) * norm_gain[None, :]).astype(jnp.bfloat16)
    shared_hidden = (jax.nn.silu(jnp.dot(normed, shared_gate, preferred_element_type=jnp.float32)) * jnp.dot(normed, shared_up, preferred_element_type=jnp.float32)).astype(jnp.bfloat16)
    shared_out = jnp.dot(shared_hidden, shared_down, preferred_element_type=jnp.float32)
    tokens_all = normed.shape[0]
    top_count = route_ids.shape[1]
    flat_ids = route_ids.reshape(-1).astype(jnp.int32)
    onehot = (flat_ids[:, None] == jnp.arange(EXPERTS, dtype=jnp.int32)[None, :]).astype(jnp.int32)
    rank_in_expert = lax.optimization_barrier(jnp.sum(jnp.cumsum(onehot, axis=0) * onehot, axis=1)) - 1
    slot_width = N_SP * N_TP * CAP
    sentinel = tokens_all * top_count
    slot_table = jnp.full((EXPERTS, slot_width), sentinel, jnp.int32).at[flat_ids, rank_in_expert].set(jnp.arange(sentinel, dtype=jnp.int32))
    extended = jnp.concatenate([normed, jnp.zeros((1, normed.shape[1]), jnp.bfloat16)], axis=0)
    weight_ext = jnp.concatenate([route_weight.reshape(-1), jnp.zeros((1,), jnp.float32)], axis=0)

    def expert_step(totals, stacked):
        gate_w, up_w, down_w, entries = stacked
        token_rows = entries // top_count
        gathered = jnp.take(extended, token_rows, axis=0)
        hidden = (jax.nn.silu(jnp.dot(gathered, gate_w, preferred_element_type=jnp.float32)) * jnp.dot(gathered, up_w, preferred_element_type=jnp.float32)).astype(jnp.bfloat16)
        produced = jnp.dot(hidden, down_w, preferred_element_type=jnp.float32).astype(jnp.bfloat16)
        weights = jnp.take(weight_ext, entries)
        return (totals.at[token_rows].add(produced.astype(jnp.float32) * weights[:, None]), None)
    start_totals = jnp.zeros((tokens_all + 1, normed.shape[1]), jnp.float32)
    routed, _ = lax.scan(expert_step, start_totals, (expert_gate, expert_up, expert_down, slot_table))
    return (middle_float + shared_out + routed[:tokens_all]).astype(jnp.bfloat16)
```

```python
import functools

import jax
import jax.numpy as jnp
from jax import lax
from jax.sharding import PartitionSpec as P

reach_rows = 8
norm_eps = 1e-06


def with_halo(cells, sides, width):
    for axis, dim in sides:
        count = lax.axis_size(axis)
        ends = count - 1
        head = lax.slice_in_dim(cells, 0, width, axis=dim)
        tail = lax.slice_in_dim(cells, cells.shape[dim] - width, cells.shape[dim], axis=dim)
        cells = jnp.concatenate(
            [
                lax.ppermute(tail, axis, [(i, (i + 1) % count) for i in range(ends)]),
                cells,
                lax.ppermute(head, axis, [((i + 1) % count, i) for i in range(ends)]),
            ],
            axis=dim,
        )
    return cells


def window_means(padded, length, offset, whole_len):
    positions = offset + lax.iota(jnp.int32, length)
    running = jnp.zeros((length,) + padded.shape[1:], jnp.float32)
    averages = []
    covered = 0
    for section_num in range(4):
        half_span = 2**section_num
        for row_shift in list(range(-half_span, -covered)) + list(range(covered, half_span)):
            running = running + padded[reach_rows + row_shift : reach_rows + row_shift + length]
        covered = half_span
        upper_end = jnp.minimum(positions + half_span, whole_len)
        lower_end = jnp.maximum(positions - half_span, 0)
        row_count = (upper_end - lower_end).astype(jnp.float32)
        averages.append(running / row_count[:, None, None])
    return averages


def arrival_plan(length):
    plan = []
    for spot in range(length):
        inner = min(spot, length - 1 - spot)
        toward_right = spot < length - 1 - spot
        row = [("own", 0)]
        for slot in range(1, length):
            if slot <= 2 * inner:
                row.append(("left" if slot % 2 else "right", (slot + 1) // 2))
            else:
                row.append(("right" if toward_right else "left", slot - inner))
        plan.append(row)
    return plan


def pick(spot, options):
    groups = {}
    for place, (key, value) in options.items():
        groups.setdefault(key, ([], value))[0].append(place)
    items = sorted(groups.values(), key=lambda item: -len(item[0]))
    result = items[0][1]
    for places, value in items[1:]:
        hit = functools.reduce(jnp.logical_or, [spot == place for place in places])
        result = jnp.where(hit, value, result)
    return result


def expert_partial(rows, width, gate, up, down, first, total):
    x = rows[:, :width]
    local = gate.shape[0]
    extra = rows[:, width:].astype(jnp.float32)
    weights = lax.dynamic_slice_in_dim(
        extra[:, :total] + extra[:, total : 2 * total], first, local, axis=1
    )
    parts = []
    for e in range(local):
        g = jnp.dot(x, gate[e], preferred_element_type=jnp.float32)
        u = jnp.dot(x, up[e], preferred_element_type=jnp.float32)
        parts.append((jax.nn.silu(g) * u * weights[:, e : e + 1]).astype(jnp.bfloat16))
    hidden = jnp.concatenate(parts, axis=1)
    flat_down = down.reshape(local * down.shape[1], down.shape[2])
    return jnp.dot(hidden, flat_down, preferred_element_type=jnp.float32).astype(jnp.bfloat16)


def routed_experts(normed, route_ids, route_weight, expert_gate, expert_up, expert_down):
    count = lax.axis_size("sp")
    pairs = 2 if count % 2 == 0 else 1
    length = count // pairs
    me = lax.axis_index("sp")
    spot = me // pairs
    local = expert_gate.shape[0]
    total = local * count
    rows_here, width = normed.shape
    names = lax.iota(jnp.int32, total)
    table = jnp.sum(
        jnp.where(route_ids[:, :, None] == names[None, None, :], route_weight[:, :, None], 0.0),
        axis=1,
    )
    coarse = table.astype(jnp.bfloat16)
    fine = (table - coarse.astype(jnp.float32)).astype(jnp.bfloat16)
    pad = -(2 * total) % 128
    chunk = jnp.concatenate(
        [normed, coarse, fine, jnp.zeros((rows_here, pad), jnp.bfloat16)], axis=1
    )
    to_right = [(i, i + pairs) for i in range(count - pairs)]
    to_left = [(i + pairs, i) for i in range(count - pairs)]
    swap = [(i, i ^ 1) for i in range(count)]

    seen = {("own", 0): chunk}
    moving_right, moving_left = chunk, chunk
    for hop in range(1, length):
        moving_right = lax.ppermute(moving_right, "sp", to_right)
        moving_left = lax.ppermute(moving_left, "sp", to_left)
        seen["left", hop] = moving_right
        seen["right", hop] = moving_left
    plan = arrival_plan(length)

    partial = []
    for slot in range(length):
        mine = pick(spot, {z: (plan[z][slot], seen[plan[z][slot]]) for z in range(length)})
        if pairs == 2:
            other = lax.ppermute(mine, "sp", swap)
            both = jnp.concatenate([mine, other], axis=0)
            result = expert_partial(
                both, width, expert_gate, expert_up, expert_down, me * local, total
            )
            back = lax.ppermute(result[rows_here:], "sp", swap)
            partial.append((result[:rows_here].astype(jnp.float32) + back.astype(jnp.float32)).astype(jnp.bfloat16))
        else:
            partial.append(
                expert_partial(
                    mine, width, expert_gate, expert_up, expert_down, me * local, total
                )
            )

    sums = partial[0].astype(jnp.float32)
    for side, perm in (("left", to_left), ("right", to_right)):
        carried = None
        for hop in range(length - 1, 0, -1):
            options = {}
            for z in range(length):
                if (side, hop) in plan[z]:
                    slot = plan[z].index((side, hop))
                    options[z] = (slot, partial[slot])
            term = pick(spot, options)
            if carried is not None:
                term = (term.astype(jnp.float32) + carried.astype(jnp.float32)).astype(jnp.bfloat16)
            carried = lax.ppermute(term, "sp", perm)
        if carried is not None:
            sums = sums + carried.astype(jnp.float32)
    return sums


def shards(
    resid,
    pool_in,
    pool_weight,
    pool_scale,
    out_weight,
    norm_gain,
    route_ids,
    route_weight,
    expert_gate,
    expert_up,
    expert_down,
    shared_gate,
    shared_up,
    shared_down,
):
    tok_local = pool_in.shape[0]
    local_groups = pool_weight.shape[0]
    group_width = pool_weight.shape[1]
    seq_total = tok_local * lax.axis_size("sp")
    padded = with_halo(pool_in, (("sp", 0),), reach_rows)
    padded = padded.astype(jnp.float32).reshape(
        tok_local + 2 * reach_rows, local_groups, group_width
    )
    averages = window_means(padded, tok_local, lax.axis_index("sp") * tok_local, seq_total)
    center = padded[reach_rows : reach_rows + tok_local]
    group_ids = lax.axis_index("tp") * local_groups + lax.iota(jnp.int32, local_groups)
    chosen = averages[0]
    for section_num in range(1, 4):
        chosen = jnp.where((group_ids == section_num)[None, :, None], averages[section_num], chosen)
    spread = (chosen - center).astype(jnp.bfloat16)
    mixed_rows = jnp.einsum("tgc,gce->tge", spread, pool_weight, preferred_element_type=jnp.float32)
    pooled = (mixed_rows.reshape(tok_local, -1) * pool_scale[None, :]).astype(jnp.bfloat16)
    token_pooled = lax.all_to_all(pooled, "tp", split_axis=0, concat_axis=1, tiled=True)
    branch = jnp.dot(
        token_pooled,
        lax.all_gather(out_weight, "tp", axis=0, tiled=True),
        preferred_element_type=jnp.float32,
    )
    middle = (resid.astype(jnp.float32) + branch).astype(jnp.bfloat16)
    middle_float = middle.astype(jnp.float32)
    square_mean = jnp.mean(middle_float * middle_float, axis=1, keepdims=True)
    normed = (middle_float * lax.rsqrt(square_mean + norm_eps) * norm_gain[None, :]).astype(
        jnp.bfloat16
    )
    shared_hidden = (
        jax.nn.silu(jnp.dot(normed, shared_gate, preferred_element_type=jnp.float32))
        * jnp.dot(normed, shared_up, preferred_element_type=jnp.float32)
    ).astype(jnp.bfloat16)
    shared_out = jnp.dot(shared_hidden, shared_down, preferred_element_type=jnp.float32)
    routed = routed_experts(
        normed, route_ids, route_weight, expert_gate, expert_up, expert_down
    )
    return (middle_float + shared_out + routed).astype(jnp.bfloat16)


def solution(mesh):
    return jax.shard_map(
        shards,
        mesh=mesh,
        in_specs=(
            P(("sp", "tp"), None),
            P("sp", "tp"),
            P("tp", None, None),
            P("tp"),
            P("tp", None),
            P(),
            P(("sp", "tp"), None),
            P(("sp", "tp"), None),
            P("sp", None, None),
            P("sp", None, None),
            P("sp", None, None),
            P(),
            P(),
            P(),
        ),
        out_specs=P(("sp", "tp"), None),
        check_vma=False,
    )
```
